32 devices in a mesh: sp: 8 (over z, y), tp: 4 (over x, core).
Axes of the slice: x: 2, y: 2, z: 4, core: 2. Of those that a mesh axis runs over, the one named last changes fastest.
Arguments:
- residual: bfloat16 [1536, 2048], P(('sp', 'tp')), may hold values from -6 to 6
- mixer_input: bfloat16 [1536, 512], P('sp', 'tp'), may hold values from -6 to 6
- log_gate: float32 [1536, 32], P('sp', 'tp'), may hold values from -2 to 0
- decay_rate: float32 [2, 32, 64], P(None, 'tp'), may hold values from 0 to 1
- turn_rate: float32 [2, 32, 64], P(None, 'tp'), may hold values from -1 to 1
- drive_real: float32 [2, 32, 16, 64], P(None, 'tp'), may hold values from -1 to 1
- drive_imaginary: float32 [2, 32, 16, 64], P(None, 'tp'), may hold values from -1 to 1
- read_real: float32 [2, 32, 16, 64], P(None, 'tp'), may hold values from -0.75 to 0.75
- read_imaginary: float32 [2, 32, 16, 64], P(None, 'tp'), may hold values from -0.75 to 0.75
- skip_gain: float32 [512], P('tp'), may hold values from -4 to 4
- project_weight: bfloat16 [512, 2048], replicated, may hold values from -0.25 to 0.25
- norm_gain: float32 [2048], replicated, may hold values from 0.1 to 1.9
- final_gain: float32 [2048], replicated, may hold values from 0.1 to 1.9
- routes: int32 [1536, 2], P('sp'), may hold values from 0 to 7, all different within a row; in each aligned block of 48 rows (0 to 47, 48 to 95, ...) at most 18 rows name the same one
- group_weight: float32 [1536], P('sp'), may hold values from 0.2 to 1
- expert_weight: float32 [1536, 2], P('sp'), may hold values from 0.1 to 1
- gate_weight: bfloat16 [8, 2048, 1024], P('sp', None, 'tp'), may hold values from -0.125 to 0.125
- linear_weight: bfloat16 [8, 2048, 1024], P('sp', None, 'tp'), may hold values from -0.125 to 0.125
- down_weight: bfloat16 [8, 1024, 2048], P('sp', 'tp'), may hold values from -0.1875 to 0.1875
Outputs:
- finished: bfloat16 [1536, 2048], P(('sp', 'tp'))
The draws below stay inside these ranges and needn't reach their ends.
Inputs may be any that keep to these rules, and one draw needn't show every extreme that they name: `routes`: each row names 2 different experts. In each aligned block of 48 rows no expert is named by more than 18 rows; some expert is named by exactly 18 rows of some block.
All inputs are finite; a program needn't handle non-finite values.
Results may differ from the reference program's by a relative error of at most 0.006.
Values may be sent and summed in bfloat16 or wider, within the bound.
A program may use at most 128 MiB of HBM per device.

```python
import math
import jax
import jax.numpy as jnp
import numpy as np
from jax import lax

D = 2048
S_GROUPS = 32
GROUP_DIM = 16
S_STATE = 64
S_WIDTH = 512
D_EXPERT = 1024
TOP_K = 2
TOK_DEV = 192
TOKENS = 1536
TOK_SHARE = 48
EXPERTS = 8
SLOTS = 18
N_SP = 8
N_TP = 4


def draw_decay_rate(key, part):
    pick_key, fast_key, slow_key = jax.random.split(key, 3)
    fast_share = 0.5
    is_fast = jax.random.uniform(pick_key, (2, S_GROUPS, 1)) < fast_share
    fast_rate = jnp.exp(jax.random.uniform(fast_key, (2, S_GROUPS, S_STATE), minval=jnp.log(0.01), maxval=jnp.log(1.0 / 30.0)))
    slow_rate = jnp.exp(jax.random.uniform(slow_key, (2, S_GROUPS, S_STATE), minval=jnp.log(0.05), maxval=jnp.log(0.3))) / TOKENS
    return jnp.where(is_fast, fast_rate, slow_rate).astype(jnp.float32)


def draw_log_gate(key, part):
    factor_key, rough_key, place_key, drop_key = jax.random.split(key, 4)
    blocks = TOKENS // TOK_DEV
    factor = jnp.exp(jax.random.uniform(factor_key, (blocks, 1, S_GROUPS), minval=0.0, maxval=jnp.log(4.0)))
    roughness = jnp.exp(0.5 * jnp.clip(jax.random.normal(rough_key, (blocks, TOK_DEV, S_GROUPS)), -3.0, 3.0))
    steady = -0.2 / TOKENS * (factor * roughness).reshape(TOKENS, S_GROUPS)
    places = jax.random.randint(place_key, (2,), 0, TOKENS)
    drop_sizes = jnp.log(jax.random.uniform(drop_key, (2, S_GROUPS), minval=0.5, maxval=0.8))
    matches = (jnp.arange(TOKENS, dtype=jnp.int32)[:, None] == places[None, :]).astype(jnp.float32)
    return (steady + jnp.dot(matches, drop_sizes, precision=lax.Precision.HIGHEST)).astype(jnp.float32)


def shard_levels(stream_key, shape, pieces, smallest, high):
    def one(axis_at, shards_of):
        draws = jax.random.uniform(jax.random.fold_in(jax.random.fold_in(stream_key, 6), axis_at), (shards_of,), jnp.float32, smallest / len(pieces), high / len(pieces))
        return jnp.repeat(jnp.exp(draws), shape[axis_at] // shards_of).reshape((-1,) + (1,) * (len(shape) - axis_at - 1))

    level = one(*pieces[0])
    for cut in pieces[1:]:
        level = level * one(*cut)
    return level


def assign_block(rng, own, number, rows, number_of, top, most, skew):
    ranking = jax.random.permutation(rng, number_of)
    heavy_load, common = shares(number_of, rows * top, most, skew, True), shares(number_of, rows * top, most, skew, False)
    places = jnp.arange(number_of)

    def named(tallies, turn):
        used = int((tallies > 0).sum())
        fixed = max(1, used // 4)
        passed = fixed + (places - fixed + turn * (used - fixed)) % max(1, number_of - fixed)
        return jnp.zeros((number_of,), jnp.int32).at[ranking[jnp.where(places < fixed, places, passed)]].set(jnp.asarray(tallies, jnp.int32))

    tallies = jnp.where(number % 4 == 0, named(heavy_load, number // 4), named(common, number - number // 4 - 1))
    mixed = jax.random.permutation(jax.random.fold_in(own, 3), number_of)
    source_of, taker = mixed[0:number_of // 2 * 2:2], mixed[1:number_of // 2 * 2:2]
    room = jnp.minimum(tallies[source_of] - 1, most - tallies[taker]) // 2
    room = jnp.where((source_of == ranking[0]) | (taker == ranking[0]) | (tallies[taker] == 0), 0, jnp.maximum(room, 0))
    passed = jax.random.randint(jax.random.fold_in(own, 4), (number_of // 2,), 0, 1 << 20) % (room + 1)
    tallies = tallies.at[source_of].add(-passed).at[taker].add(passed)
    labels = jnp.searchsorted(jnp.cumsum(tallies), jnp.arange(rows * top), side="right").astype(jnp.int32)
    table = labels.reshape(top, rows).T
    table = table[jax.random.permutation(jax.random.fold_in(own, 1), rows)]
    turn = jax.random.randint(jax.random.fold_in(own, 2), (rows, 1), 0, top)
    return jnp.take_along_axis(table, (jnp.arange(top)[None, :] + turn) % top, axis=1)


def shares(count, total, limit, slope, full):
    weights = [(1 << 20) // math.isqrt(grade ** slope) + 1 for grade in range(1, count + 1)]
    largest = limit if full else min(limit, max(-(-total // count), total * weights[0] // sum(weights)))
    least = 1 if total - largest >= count - 1 else 0
    given, surplus = [largest] + [least] * (count - 1), total - largest - least * (count - 1)
    while surplus > 0:
        candidates = [i for i in range(1, count) if given[i] < largest] or [i for i in range(1, count) if given[i] < limit]
        pool, budget = sum([weights[i] for i in candidates]), surplus
        for i in candidates:
            extra = min(limit - given[i], max(1, budget * weights[i] // pool), surplus)
            given[i] = given[i] + extra
            surplus = surplus - extra
    return np.array(given)


def centred(key, extent, width, most, cuts=(), kind=jnp.bfloat16):
    drawn = width * jax.random.normal(key, extent, jnp.float32)
    if cuts:
        drawn = drawn * shard_levels(key, extent, cuts, -0.22, 0.18)
    return jnp.clip(drawn, -most, most).astype(kind)


def setup_inputs(seed: int = 0) -> dict:
    key_list = jax.random.split(jax.random.key(seed), 20)
    residual = centred(key_list[0], (TOKENS, D), 1.0, 6.0, ((0, 32),))
    mixer_input = centred(key_list[1], (TOKENS, S_WIDTH), 1.0, 6.0, ((0, 8), (1, 4)))
    log_gate = draw_log_gate(jax.random.fold_in(key_list[19], 71), 0)
    decay_rate = draw_decay_rate(jax.random.fold_in(key_list[19], 71), 0)
    turn_rate = jnp.clip(jax.random.uniform(key_list[4], (2, S_GROUPS, S_STATE), jnp.float32, -1.0, 1.0) * shard_levels(key_list[4], (2, S_GROUPS, S_STATE), ((1, 4),), -0.4, 0.0), -1.0, 1.0)
    drive_real = centred(key_list[5], (2, S_GROUPS, GROUP_DIM, S_STATE), (2 * GROUP_DIM) ** -0.5, 1.0, ((1, 4),), jnp.float32)
    drive_imaginary = centred(key_list[6], (2, S_GROUPS, GROUP_DIM, S_STATE), (2 * GROUP_DIM) ** -0.5, 1.0, ((1, 4),), jnp.float32)
    read_real = centred(key_list[7], (2, S_GROUPS, GROUP_DIM, S_STATE), S_STATE ** -0.5, 0.75, ((1, 4),), jnp.float32)
    read_imaginary = centred(key_list[8], (2, S_GROUPS, GROUP_DIM, S_STATE), S_STATE ** -0.5, 0.75, ((1, 4),), jnp.float32)
    skip_gain = centred(key_list[9], (S_WIDTH,), 1.0, 4.0, ((0, 4),), jnp.float32)
    project_weight = centred(key_list[10], (S_WIDTH, D), S_WIDTH ** -0.5, 0.25)
    norm_gain = jnp.clip(1.0 + 0.18 * jax.random.normal(key_list[11], (D,), jnp.float32), 0.1, 1.9)
    final_gain = jnp.clip(1.0 + 0.18 * jax.random.normal(key_list[12], (D,), jnp.float32), 0.1, 1.9)
    routes_keys = jax.random.split(jax.random.fold_in(key_list[13], 1), TOKENS // TOK_SHARE)
    routes_turns = jax.random.permutation(jax.random.fold_in(key_list[13], 3), TOKENS // TOK_SHARE)
    routes = jax.vmap(lambda own, number: assign_block(jax.random.fold_in(key_list[13], 2), own, number, TOK_SHARE, EXPERTS, TOP_K, SLOTS, 2))(routes_keys, routes_turns).reshape((TOKENS, TOP_K))
    group_weight = jnp.clip(jnp.exp(math.log(1.0) - 1.609438 * jax.random.uniform(key_list[14], (TOKENS,), jnp.float32) ** shard_levels(key_list[14], (TOKENS,), ((0, 8),), -0.2, 0.2)), 0.2, 1.0)
    expert_weight = jnp.clip(jnp.exp(math.log(1.0) - 2.3025851 * jax.random.uniform(key_list[15], (TOKENS, TOP_K), jnp.float32) ** shard_levels(key_list[15], (TOKENS, TOP_K), ((0, 8),), -0.2, 0.2)), 0.1, 1.0)
    gate_weight = centred(key_list[16], (EXPERTS, D, D_EXPERT), D ** -0.5, 0.125, ((0, 8), (2, 4)))
    linear_weight = centred(key_list[17], (EXPERTS, D, D_EXPERT), D ** -0.5, 0.125, ((0, 8), (2, 4)))
    down_weight = centred(key_list[18], (EXPERTS, D_EXPERT, D), D_EXPERT ** -0.5, 0.1875, ((0, 8), (1, 4)))
    return {"residual": residual, "mixer_input": mixer_input, "log_gate": log_gate, "decay_rate": decay_rate, "turn_rate": turn_rate, "drive_real": drive_real, "drive_imaginary": drive_imaginary, "read_real": read_real, "read_imaginary": read_imaginary, "skip_gain": skip_gain, "project_weight": project_weight, "norm_gain": norm_gain, "final_gain": final_gain, "routes": routes, "group_weight": group_weight, "expert_weight": expert_weight, "gate_weight": gate_weight, "linear_weight": linear_weight, "down_weight": down_weight}


deep_alpha = 2.0 ** 0.25
norm_epsilon = 1e-05
highest = lax.Precision.HIGHEST

def layer_norm(values, gain):
    center = values - lax.optimization_barrier(jnp.mean(values, axis=-1, keepdims=True))
    spread = lax.optimization_barrier(jnp.mean(center * center, axis=-1, keepdims=True))
    return center * lax.rsqrt(spread + norm_epsilon) * gain

def sweep(inputs, log_gate, rate_row, turn_row, drive_real, drive_imaginary, read_real, read_imaginary, backward):
    input_scale = jnp.sqrt(1.0 - jnp.exp(-2.0 * rate_row))
    retain = jnp.exp(-rate_row)
    step_real = retain * jnp.cos(turn_row)
    step_imaginary = retain * jnp.sin(turn_row)

    def advance(carried, current):
        state_real, state_imaginary = carried
        token_row, gate_row = current
        push_real = jnp.einsum('gh,ghp->gp', token_row, drive_real, precision=highest) * input_scale
        push_imaginary = jnp.einsum('gh,ghp->gp', token_row, drive_imaginary, precision=highest) * input_scale
        factor = jnp.exp(gate_row)[:, None]
        new_real = factor * (step_real * state_real - step_imaginary * state_imaginary) + push_real
        new_imaginary = factor * (step_real * state_imaginary + step_imaginary * state_real) + push_imaginary
        output = jnp.einsum('gp,ghp->gh', new_real, read_real, precision=highest) - jnp.einsum('gp,ghp->gh', new_imaginary, read_imaginary, precision=highest)
        return ((new_real, new_imaginary), output)
    initial = jnp.zeros(rate_row.shape, jnp.float32)
    _, outputs = lax.scan(advance, (initial, initial), (inputs, log_gate), reverse=backward)
    return outputs

def reference(residual, mixer_input, log_gate, decay_rate, turn_rate, drive_real, drive_imaginary, read_real, read_imaginary, skip_gain, project_weight, norm_gain, final_gain, routes, group_weight, expert_weight, gate_weight, linear_weight, down_weight):
    inputs = mixer_input.astype(jnp.float32).reshape(TOKENS, S_GROUPS, GROUP_DIM)
    readout = sweep(inputs, log_gate, decay_rate[0], turn_rate[0], drive_real[0], drive_imaginary[0], read_real[0], read_imaginary[0], False)
    readout = readout + sweep(inputs, log_gate, decay_rate[1], turn_rate[1], drive_real[1], drive_imaginary[1], read_real[1], read_imaginary[1], True)
    readout = readout + skip_gain.reshape(S_GROUPS, GROUP_DIM) * inputs
    activated = jax.nn.gelu(readout).reshape(TOKENS, S_WIDTH).astype(jnp.bfloat16)
    branch = jnp.dot(activated, project_weight, preferred_element_type=jnp.float32)
    middle = layer_norm(deep_alpha * residual.astype(jnp.float32) + branch, norm_gain)
    middle_rows = middle.astype(jnp.bfloat16)
    flat_experts = routes.reshape(-1)
    sorted_order = jnp.argsort(flat_experts, stable=True).astype(jnp.int32)
    counts = lax.optimization_barrier(jnp.sum((flat_experts[:, None] == jnp.arange(EXPERTS, dtype=jnp.int32)[None, :]).astype(jnp.int32), axis=0))
    starts = (jnp.cumsum(counts) - counts).astype(jnp.int32)
    capacity = N_SP * N_TP * SLOTS
    assigned = TOKENS * TOP_K
    piece_width = D_EXPERT // N_TP

    def run_expert(expert):
        offsets = jnp.arange(capacity, dtype=jnp.int32)
        is_valid = offsets < counts[expert]
        chosen = sorted_order[jnp.minimum(starts[expert] + offsets, assigned - 1)]
        row_inputs = middle_rows[chosen // TOP_K]
        gate_part = jnp.dot(row_inputs, gate_weight[expert], preferred_element_type=jnp.float32)
        linear_part = jnp.dot(row_inputs, linear_weight[expert], preferred_element_type=jnp.float32)
        hidden = (jax.nn.silu(gate_part) * linear_part).astype(jnp.bfloat16)
        running = jnp.zeros((capacity, D), jnp.float32)
        for member in range(N_TP):
            partial_value = jnp.dot(hidden[:, member * piece_width:(member + 1) * piece_width], down_weight[expert, member * piece_width:(member + 1) * piece_width], preferred_element_type=jnp.float32)
            rounded = lax.optimization_barrier(partial_value.astype(jnp.bfloat16))
            running = running + rounded.astype(jnp.float32)
        return (running.astype(jnp.bfloat16), jnp.where(is_valid, chosen, assigned).astype(jnp.int32))
    results, targets = lax.map(run_expert, jnp.arange(EXPERTS, dtype=jnp.int32))
    answers = jnp.zeros((assigned, D), jnp.bfloat16).at[targets.reshape(-1)].set(results.reshape(-1, D), mode='drop')
    mixing = group_weight[:, None] * expert_weight / lax.optimization_barrier(jnp.sum(expert_weight, axis=1, keepdims=True))
    routed = lax.optimization_barrier(jnp.sum(mixing[:, :, None] * answers.reshape(TOKENS, TOP_K, D).astype(jnp.float32), axis=1))
    finished = layer_norm(deep_alpha * middle + routed, final_gain)
    return finished.astype(jnp.bfloat16)
```

```python
import functools

import jax
import jax.numpy as jnp
from jax import lax
from jax.experimental import pallas as pl
from jax.experimental.pallas import tpu as pltpu
from jax.sharding import PartitionSpec as P

deep_alpha = 2.0**0.25
norm_epsilon = 1e-05
highest = lax.Precision.HIGHEST
f32 = jnp.float32
bf16 = jnp.bfloat16
segments = 8


def layer_norm(values, gain):
    center = values - jnp.mean(values, axis=-1, keepdims=True)
    spread = jnp.mean(center * center, axis=-1, keepdims=True)
    return center * lax.rsqrt(spread + norm_epsilon) * gain


def iota(shape, axis):
    return lax.broadcasted_iota(jnp.int32, shape, axis)


def exact_dot(a, b, dims=((1,), (0,))):
    return lax.dot_general(a, b, (dims, ((), ())), precision=highest, preferred_element_type=f32)


def mixer_kernel(
    n_sp,
    n_tp,
    x_ref,
    gate_ref,
    decay_ref,
    turn_ref,
    drive_re,
    drive_im,
    read_re,
    read_im,
    skip_ref,
    weight_hbm,
    residual_ref,
    gain_ref,
    middle_ref,
    push,
    gate,
    seg,
    enter,
    total,
    totals,
    act,
    chan,
    weight,
    weight_sem,
    send_a,
    recv_a,
    send_b,
    recv_b,
):
    sp = lax.axis_index("sp")
    tp = lax.axis_index("tp")
    barrier = pltpu.get_barrier_semaphore()
    for k in range(1, n_sp):
        pl.semaphore_signal(barrier, inc=1, device_id={"sp": lax.rem(sp + k, n_sp)})
    for k in range(1, n_tp):
        pl.semaphore_signal(barrier, inc=1, device_id={"tp": lax.rem(tp + k, n_tp)})
    fetch = pltpu.make_async_copy(weight_hbm, weight, weight_sem)
    fetch.start()

    length, channels = x_ref.shape
    groups, states = decay_ref.shape[1:]
    width = groups * states
    each = channels // groups
    steps = length // segments
    order = iota((length, length), 0)
    place = iota((length, length), 1)
    shuffle = (place == (order % segments) * steps + order // segments).astype(f32)
    x = jnp.dot(shuffle.astype(bf16), x_ref[...], preferred_element_type=f32)
    spread = (iota((states, width), 1) % states == iota((states, width), 0)).astype(f32)
    own = iota((groups, width), 1) // states == iota((groups, width), 0)
    diagonal = iota((channels, width), 1) // states == iota((channels, width), 0) // each

    def row(values):
        wide = exact_dot(values, spread)
        return jnp.sum(jnp.where(own, wide, 0.0), axis=0, keepdims=True)

    def table(values):
        return jnp.where(diagonal, exact_dot(values, spread), 0.0)

    gate[...] = exact_dot(exact_dot(shuffle, jnp.exp(gate_ref[...])), own.astype(f32))
    turn_rows = []
    for k in range(2):
        rate = decay_ref[k]
        turn = turn_ref[k]
        retain = jnp.exp(-rate)
        scale = row(jnp.sqrt(1.0 - jnp.exp(-2.0 * rate)))
        turn_rows.append((row(retain * jnp.cos(turn)), row(retain * jnp.sin(turn))))
        push[2 * k] = exact_dot(x, table(drive_re[k]) * scale)
        push[2 * k + 1] = exact_dot(x, table(drive_im[k]) * scale)
    (f_re, f_im), (b_re, b_im) = turn_rows

    zero = jnp.zeros((segments, width), f32)
    one = jnp.ones((segments, width), f32)

    def rows_of(j):
        return pl.ds(pl.multiple_of(j * segments, segments), segments)

    def first(j, c):
        out = []
        for k, (sr, si) in enumerate(((f_re, f_im), (b_re, b_im))):
            at = rows_of(j if k == 0 else steps - 1 - j)
            ar, ai, vr, vi = c[4 * k : 4 * k + 4]
            g = gate[at, :]
            mr, mi = g * sr, g * si
            out += [
                mr * ar - mi * ai,
                mr * ai + mi * ar,
                mr * vr - mi * vi + push[2 * k, at, :],
                mr * vi + mi * vr + push[2 * k + 1, at, :],
            ]
        return tuple(out)

    ends = lax.fori_loop(0, steps, first, (one, zero, zero, zero) * 2)
    for i, part in enumerate(ends):
        seg[i] = part

    def link(parts, c):
        ar, ai, vr, vi = parts
        return (ar * c[0] - ai * c[1] + vr, ar * c[1] + ai * c[0] + vi)

    def seg_rows(k, s):
        return [seg[4 * k + i, s : s + 1, :] for i in range(4)]

    for k in range(2):
        span = range(segments) if k == 0 else range(segments - 1, -1, -1)
        decay = (one[:1], zero[:1])
        state = (zero[:1], zero[:1])
        for s in span:
            parts = seg_rows(k, s)
            state = link(parts, state)
            decay = link(parts[:2] + [0.0, 0.0], decay)
        for i, value in enumerate(decay + state):
            total[4 * k + i : 4 * k + i + 1, :] = value
    totals[sp] = total[...]

    pl.semaphore_wait(barrier, n_sp - 1 + n_tp - 1)

    def hand(k):
        peer = lax.rem(sp + k, n_sp)
        return pltpu.make_async_remote_copy(
            src_ref=total,
            dst_ref=totals.at[sp],
            send_sem=send_a.at[k],
            recv_sem=recv_a.at[sp],
            device_id={"sp": peer},
        )

    def arrival(k):
        source = lax.rem(sp + k, n_sp)
        return pltpu.make_async_remote_copy(
            src_ref=total,
            dst_ref=totals.at[source],
            send_sem=send_a.at[k],
            recv_sem=recv_a.at[source],
            device_id={"sp": source},
        )

    for k in range(1, n_sp):
        hand(k).start()
    tables = [(table(read_re[k]), table(read_im[k])) for k in range(2)]
    for k in range(1, n_sp):
        arrival(k).wait_recv()

    for k in range(2):
        c = (zero[:1], zero[:1])
        for d in range(n_sp) if k == 0 else range(n_sp - 1, -1, -1):
            new = link([totals[d, 4 * k + i : 4 * k + i + 1, :] for i in range(4)], c)
            counts = d < sp if k == 0 else d > sp
            c = tuple(jnp.where(counts, a, b) for a, b in zip(new, c))
        for s in range(segments) if k == 0 else range(segments - 1, -1, -1):
            enter[2 * k, s : s + 1, :] = c[0]
            enter[2 * k + 1, s : s + 1, :] = c[1]
            c = link(seg_rows(k, s), c)

    def second(j, c):
        out = []
        for k, (sr, si) in enumerate(((f_re, f_im), (b_re, b_im))):
            at = rows_of(j if k == 0 else steps - 1 - j)
            vr, vi = c[2 * k : 2 * k + 2]
            g = gate[at, :]
            mr, mi = g * sr, g * si
            new_re = mr * vr - mi * vi + push[2 * k, at, :]
            new_im = mr * vi + mi * vr + push[2 * k + 1, at, :]
            push[2 * k, at, :] = new_re
            push[2 * k + 1, at, :] = new_im
            out += [new_re, new_im]
        return tuple(out)

    lax.fori_loop(0, steps, second, tuple(enter[i] for i in range(4)))
    over = ((1,), (1,))
    readout = exact_dot(push[0], tables[0][0], over) - exact_dot(push[1], tables[0][1], over)
    readout = readout + (
        exact_dot(push[2], tables[1][0], over) - exact_dot(push[3], tables[1][1], over)
    )
    readout = readout + skip_ref[...] * x
    mixed = jax.nn.gelu(readout).astype(bf16)
    act[...] = lax.dot_general(
        shuffle.astype(bf16), mixed, (((0,), (0,)), ((), ())), preferred_element_type=f32
    ).astype(bf16)

    share = length // n_tp

    def shift(k, out):
        peer = lax.rem(tp + k, n_tp)
        return pltpu.make_async_remote_copy(
            src_ref=act.at[pl.ds(pl.multiple_of(peer * share, share), share)],
            dst_ref=chan.at[tp if out else peer],
            send_sem=send_b.at[k],
            recv_sem=recv_b.at[tp if out else peer],
            device_id={"tp": peer},
        )

    for k in range(1, n_tp):
        shift(k, True).start()
    chan[tp] = act[pl.ds(pl.multiple_of(tp * share, share), share), :]
    fetch.wait()
    for k in range(1, n_tp):
        shift(k, False).wait_recv()
    whole = jnp.concatenate([chan[m] for m in range(n_tp)], axis=1)
    branch = jnp.dot(whole, weight[...], preferred_element_type=f32)
    middle_ref[...] = layer_norm(
        deep_alpha * residual_ref[...].astype(f32) + branch, gain_ref[...]
    )
    for k in range(1, n_sp):
        hand(k).wait_send()
    for k in range(1, n_tp):
        shift(k, True).wait_send()


def mixer(args, n_sp, n_tp):
    (residual, x, log_gate, decay, turn, d_re, d_im, r_re, r_im, skip, weight, gain) = args
    length, channels = x.shape
    groups, states = decay.shape[1:]
    width = groups * states
    share, model = residual.shape
    flat = lambda a: a.reshape(2, channels, states)
    vmem = pl.BlockSpec(memory_space=pltpu.VMEM)
    dma = pltpu.SemaphoreType.DMA
    return pl.pallas_call(
        functools.partial(mixer_kernel, n_sp, n_tp),
        out_shape=jax.ShapeDtypeStruct((share, model), f32),
        in_specs=[vmem] * 9 + [pl.BlockSpec(memory_space=pl.ANY)] + [vmem] * 2,
        out_specs=vmem,
        scratch_shapes=[
            pltpu.VMEM((4, length, width), f32),
            pltpu.VMEM((length, width), f32),
            pltpu.VMEM((8, segments, width), f32),
            pltpu.VMEM((4, segments, width), f32),
            pltpu.VMEM((8, width), f32),
            pltpu.VMEM((n_sp, 8, width), f32),
            pltpu.VMEM((length, channels), bf16),
            pltpu.VMEM((n_tp, share, channels), bf16),
            pltpu.VMEM(weight.shape, bf16),
            dma(()),
            dma((n_sp,)),
            dma((n_sp,)),
            dma((n_tp,)),
            dma((n_tp,)),
        ],
        compiler_params=pltpu.CompilerParams(
            collective_id=0, has_side_effects=True, vmem_limit_bytes=40 * 2**20
        ),
        name="mixer",
    )(
        x,
        log_gate,
        decay,
        turn,
        flat(d_re),
        flat(d_im),
        flat(r_re),
        flat(r_im),
        skip[None, :],
        weight,
        residual,
        gain[None, :],
    )


def on_device(
    residual,
    mixer_input,
    log_gate,
    decay_rate,
    turn_rate,
    drive_real,
    drive_imaginary,
    read_real,
    read_imaginary,
    skip_gain,
    project_weight,
    norm_gain,
    final_gain,
    routes,
    group_weight,
    expert_weight,
    gate_weight,
    linear_weight,
    down_weight,
):
    experts = lax.axis_size("sp")
    members = lax.axis_size("tp")
    member = lax.axis_index("tp")
    middle = mixer(
        (
            residual,
            mixer_input,
            log_gate,
            decay_rate,
            turn_rate,
            drive_real,
            drive_imaginary,
            read_real,
            read_imaginary,
            skip_gain,
            project_weight,
            norm_gain,
        ),
        experts,
        members,
    )
    middle_rows = middle.astype(bf16)
    share, model = middle.shape
    top = routes.shape[1]
    slots = max(2, 3 * share * top // (2 * experts))
    mixing = group_weight[:, None] * expert_weight / jnp.sum(expert_weight, axis=1, keepdims=True)
    mine = lax.dynamic_slice_in_dim(routes, member * share, share, 0)
    own_mixing = lax.dynamic_slice_in_dim(mixing, member * share, share, 0)
    named = mine[:, :, None] == jnp.arange(experts)[None, None, :]
    uses = jnp.any(named, axis=1)
    earlier = jnp.arange(share)[None, :] < jnp.arange(share)[:, None]
    rank = jnp.dot(earlier.astype(bf16), uses.astype(bf16), preferred_element_type=f32)
    chosen = uses[:, :, None] & (rank[:, :, None] == jnp.arange(slots).astype(f32))
    outgoing = jnp.einsum(
        "nes,nd->esd", chosen.astype(bf16), middle_rows, preferred_element_type=f32
    ).astype(bf16)
    landed = lax.all_to_all(outgoing, "sp", split_axis=0, concat_axis=0, tiled=True)
    arrived = lax.all_gather(landed[None], "tp", axis=0, tiled=True)
    expert_input = arrived.reshape(-1, model)
    gate_part = jnp.dot(expert_input, gate_weight[0], preferred_element_type=f32)
    linear_part = jnp.dot(expert_input, linear_weight[0], preferred_element_type=f32)
    hidden = (jax.nn.silu(gate_part) * linear_part).astype(bf16)
    summed = lax.psum_scatter(
        jnp.dot(hidden, down_weight[0], preferred_element_type=f32).astype(bf16),
        "tp",
        scatter_dimension=0,
        tiled=True,
    )
    answers = summed.reshape(experts, slots, model)
    returned = lax.all_to_all(answers, "sp", split_axis=0, concat_axis=0, tiled=True)
    share_of = jnp.sum(jnp.where(named, own_mixing[:, :, None], 0.0), axis=1)
    weigh = jnp.where(chosen, share_of[:, :, None], 0.0)
    coarse = weigh.astype(bf16)
    fine = (weigh - coarse.astype(f32)).astype(bf16)
    routed = jnp.einsum(
        "nes,esd->nd", jnp.concatenate([coarse, fine]), returned, preferred_element_type=f32
    )
    routed = routed[:share] + routed[share:]
    finished = layer_norm(deep_alpha * middle + routed, final_gain)
    return finished.astype(bf16)


def solution(mesh):
    placed = (
        P(("sp", "tp"), None),
        P("sp", "tp"),
        P("sp", "tp"),
        P(None, "tp", None),
        P(None, "tp", None),
        P(None, "tp", None, None),
        P(None, "tp", None, None),
        P(None, "tp", None, None),
        P(None, "tp", None, None),
        P("tp"),
        P(),
        P(),
        P(),
        P("sp", None),
        P("sp"),
        P("sp", None),
        P("sp", None, "tp"),
        P("sp", None, "tp"),
        P("sp", "tp", None),
    )
    return jax.shard_map(
        on_device, mesh=mesh, in_specs=placed, out_specs=P(("sp", "tp"), None), check_vma=False
    )
```

```python
import functools

import jax
import jax.numpy as jnp
from jax import lax
from jax.experimental import pallas as pl
from jax.experimental.pallas import tpu as pltpu
from jax.sharding import PartitionSpec as P

deep_alpha = 2.0**0.25
norm_epsilon = 1e-05
highest = lax.Precision.HIGHEST
f32 = jnp.float32
bf16 = jnp.bfloat16
segments = 8


def layer_norm(values, gain):
    center = values - jnp.mean(values, axis=-1, keepdims=True)
    spread = jnp.mean(center * center, axis=-1, keepdims=True)
    return center * lax.rsqrt(spread + norm_epsilon) * gain


def iota(shape, axis):
    return lax.broadcasted_iota(jnp.int32, shape, axis)


def exact_dot(a, b, dims=((1,), (0,))):
    return lax.dot_general(a, b, (dims, ((), ())), precision=highest, preferred_element_type=f32)


def mixer_kernel(
    n_sp,
    n_tp,
    x_ref,
    gate_ref,
    decay_ref,
    turn_ref,
    drive_re,
    drive_im,
    read_re,
    read_im,
    skip_ref,
    weight_hbm,
    residual_ref,
    gain_ref,
    middle_ref,
    push,
    gate,
    seg,
    enter,
    total,
    totals,
    act,
    chan,
    weight,
    weight_sem,
    send_a,
    recv_a,
    send_b,
    recv_b,
):
    sp = lax.axis_index("sp")
    tp = lax.axis_index("tp")
    barrier = pltpu.get_barrier_semaphore()
    for k in range(1, n_sp):
        pl.semaphore_signal(barrier, inc=1, device_id={"sp": lax.rem(sp + k, n_sp)})
    for k in range(1, n_tp):
        pl.semaphore_signal(barrier, inc=1, device_id={"tp": lax.rem(tp + k, n_tp)})
    fetch = pltpu.make_async_copy(weight_hbm, weight, weight_sem)
    fetch.start()

    length, channels = x_ref.shape
    groups, states = decay_ref.shape[1:]
    width = groups * states
    each = channels // groups
    steps = length // segments
    order = iota((length, length), 0)
    place = iota((length, length), 1)
    shuffle = (place == (order % segments) * steps + order // segments).astype(f32)
    x = jnp.dot(shuffle.astype(bf16), x_ref[...], preferred_element_type=f32)
    spread = (iota((states, width), 1) % states == iota((states, width), 0)).astype(f32)
    own = iota((groups, width), 1) // states == iota((groups, width), 0)
    diagonal = iota((channels, width), 1) // states == iota((channels, width), 0) // each

    def row(values):
        wide = exact_dot(values, spread)
        return jnp.sum(jnp.where(own, wide, 0.0), axis=0, keepdims=True)

    def table(values):
        return jnp.where(diagonal, exact_dot(values, spread), 0.0)

    gate[...] = exact_dot(exact_dot(shuffle, jnp.exp(gate_ref[...])), own.astype(f32))
    turn_rows = []
    for k in range(2):
        rate = decay_ref[k]
        turn = turn_ref[k]
        retain = jnp.exp(-rate)
        scale = row(jnp.sqrt(1.0 - jnp.exp(-2.0 * rate)))
        turn_rows.append((row(retain * jnp.cos(turn)), row(retain * jnp.sin(turn))))
        push[2 * k] = exact_dot(x, table(drive_re[k]) * scale)
        push[2 * k + 1] = exact_dot(x, table(drive_im[k]) * scale)
    (f_re, f_im), (b_re, b_im) = turn_rows

    zero = jnp.zeros((segments, width), f32)
    one = jnp.ones((segments, width), f32)

    def rows_of(j):
        return pl.ds(pl.multiple_of(j * segments, segments), segments)

    def first(j, c):
        out = []
        for k, (sr, si) in enumerate(((f_re, f_im), (b_re, b_im))):
            at = rows_of(j if k == 0 else steps - 1 - j)
            ar, ai, vr, vi = c[4 * k : 4 * k + 4]
            g = gate[at, :]
            mr, mi = g * sr, g * si
            out += [
                mr * ar - mi * ai,
                mr * ai + mi * ar,
                mr * vr - mi * vi + push[2 * k, at, :],
                mr * vi + mi * vr + push[2 * k + 1, at, :],
            ]
        return tuple(out)

    ends = lax.fori_loop(0, steps, first, (one, zero, zero, zero) * 2)
    for i, part in enumerate(ends):
        seg[i] = part

    def link(parts, c):
        ar, ai, vr, vi = parts
        return (ar * c[0] - ai * c[1] + vr, ar * c[1] + ai * c[0] + vi)

    def seg_rows(k, s):
        return [seg[4 * k + i, s : s + 1, :] for i in range(4)]

    for k in range(2):
        span = range(segments) if k == 0 else range(segments - 1, -1, -1)
        decay = (one[:1], zero[:1])
        state = (zero[:1], zero[:1])
        for s in span:
            parts = seg_rows(k, s)
            state = link(parts, state)
            decay = link(parts[:2] + [0.0, 0.0], decay)
        for i, value in enumerate(decay + state):
            total[4 * k + i : 4 * k + i + 1, :] = value
    totals[sp] = total[...]

    pl.semaphore_wait(barrier, n_sp - 1 + n_tp - 1)

    def hand(k):
        peer = lax.rem(sp + k, n_sp)
        return pltpu.make_async_remote_copy(
            src_ref=total,
            dst_ref=totals.at[sp],
            send_sem=send_a.at[k],
            recv_sem=recv_a.at[sp],
            device_id={"sp": peer},
        )

    def arrival(k):
        source = lax.rem(sp + k, n_sp)
        return pltpu.make_async_remote_copy(
            src_ref=total,
            dst_ref=totals.at[source],
            send_sem=send_a.at[k],
            recv_sem=recv_a.at[source],
            device_id={"sp": source},
        )

    for k in range(1, n_sp):
        hand(k).start()
    tables = [(table(read_re[k]), table(read_im[k])) for k in range(2)]
    for k in range(1, n_sp):
        arrival(k).wait_recv()

    for k in range(2):
        c = (zero[:1], zero[:1])
        for d in range(n_sp) if k == 0 else range(n_sp - 1, -1, -1):
            new = link([totals[d, 4 * k + i : 4 * k + i + 1, :] for i in range(4)], c)
            counts = d < sp if k == 0 else d > sp
            c = tuple(jnp.where(counts, a, b) for a, b in zip(new, c))
        for s in range(segments) if k == 0 else range(segments - 1, -1, -1):
            enter[2 * k, s : s + 1, :] = c[0]
            enter[2 * k + 1, s : s + 1, :] = c[1]
            c = link(seg_rows(k, s), c)

    def second(j, c):
        out = []
        for k, (sr, si) in enumerate(((f_re, f_im), (b_re, b_im))):
            at = rows_of(j if k == 0 else steps - 1 - j)
            vr, vi = c[2 * k : 2 * k + 2]
            g = gate[at, :]
            mr, mi = g * sr, g * si
            new_re = mr * vr - mi * vi + push[2 * k, at, :]
            new_im = mr * vi + mi * vr + push[2 * k + 1, at, :]
            push[2 * k, at, :] = new_re
            push[2 * k + 1, at, :] = new_im
            out += [new_re, new_im]
        return tuple(out)

    lax.fori_loop(0, steps, second, tuple(enter[i] for i in range(4)))
    over = ((1,), (1,))
    readout = exact_dot(push[0], tables[0][0], over) - exact_dot(push[1], tables[0][1], over)
    readout = readout + (
        exact_dot(push[2], tables[1][0], over) - exact_dot(push[3], tables[1][1], over)
    )
    readout = readout + skip_ref[...] * x
    mixed = jax.nn.gelu(readout).astype(bf16)
    act[...] = lax.dot_general(
        shuffle.astype(bf16), mixed, (((0,), (0,)), ((), ())), preferred_element_type=f32
    ).astype(bf16)

    share = length // n_tp

    def shift(k, out):
        peer = lax.rem(tp + k, n_tp)
        return pltpu.make_async_remote_copy(
            src_ref=act.at[pl.ds(pl.multiple_of(peer * share, share), share)],
            dst_ref=chan.at[tp if out else peer],
            send_sem=send_b.at[k],
            recv_sem=recv_b.at[tp if out else peer],
            device_id={"tp": peer},
        )

    for k in range(1, n_tp):
        shift(k, True).start()
    chan[tp] = act[pl.ds(pl.multiple_of(tp * share, share), share), :]
    fetch.wait()
    for k in range(1, n_tp):
        shift(k, False).wait_recv()
    whole = jnp.concatenate([chan[m] for m in range(n_tp)], axis=1)
    branch = jnp.dot(whole, weight[...], preferred_element_type=f32)
    middle_ref[...] = layer_norm(
        deep_alpha * residual_ref[...].astype(f32) + branch, gain_ref[...]
    )
    for k in range(1, n_sp):
        hand(k).wait_send()
    for k in range(1, n_tp):
        shift(k, True).wait_send()


def mixer(args, n_sp, n_tp):
    (residual, x, log_gate, decay, turn, d_re, d_im, r_re, r_im, skip, weight, gain) = args
    length, channels = x.shape
    groups, states = decay.shape[1:]
    width = groups * states
    share, model = residual.shape
    flat = lambda a: a.reshape(2, channels, states)
    vmem = pl.BlockSpec(memory_space=pltpu.VMEM)
    dma = pltpu.SemaphoreType.DMA
    return pl.pallas_call(
        functools.partial(mixer_kernel, n_sp, n_tp),
        out_shape=jax.ShapeDtypeStruct((share, model), f32),
        in_specs=[vmem] * 9 + [pl.BlockSpec(memory_space=pl.ANY)] + [vmem] * 2,
        out_specs=vmem,
        scratch_shapes=[
            pltpu.VMEM((4, length, width), f32),
            pltpu.VMEM((length, width), f32),
            pltpu.VMEM((8, segments, width), f32),
            pltpu.VMEM((4, segments, width), f32),
            pltpu.VMEM((8, width), f32),
            pltpu.VMEM((n_sp, 8, width), f32),
            pltpu.VMEM((length, channels), bf16),
            pltpu.VMEM((n_tp, share, channels), bf16),
            pltpu.VMEM(weight.shape, bf16),
            dma(()),
            dma((n_sp,)),
            dma((n_sp,)),
            dma((n_tp,)),
            dma((n_tp,)),
        ],
        compiler_params=pltpu.CompilerParams(
            collective_id=0, has_side_effects=True, vmem_limit_bytes=40 * 2**20
        ),
        name="mixer",
    )(
        x,
        log_gate,
        decay,
        turn,
        flat(d_re),
        flat(d_im),
        flat(r_re),
        flat(r_im),
        skip[None, :],
        weight,
        residual,
        gain[None, :],
    )


def experts_kernel(
    n_sp,
    n_tp,
    middle_ref,
    meta_ref,
    gain_ref,
    gate_hbm,
    linear_hbm,
    down_hbm,
    out_ref,
    rows_out,
    recv,
    part,
    sib,
    pair,
    peer_sum,
    final,
    back,
    gate_w,
    linear_w,
    down_w,
    weight_sems,
    s1,
    r1,
    s2x,
    s2d,
    r2,
    s3,
    r3,
    s4,
    r4,
    s5,
    r5,
):
    sp = lax.axis_index("sp")
    tp = lax.axis_index("tp")
    n_hi = n_tp // 2
    hi = tp // 2
    lo = tp % 2
    sibling = hi * 2 + 1 - lo
    barrier = pltpu.get_barrier_semaphore()
    for k in range(1, n_sp):
        pl.semaphore_signal(barrier, inc=1, device_id={"sp": lax.rem(sp + k, n_sp)})
    for k in range(1, n_tp):
        pl.semaphore_signal(barrier, inc=1, device_id={"tp": lax.rem(tp + k, n_tp)})
    fetches = [
        pltpu.make_async_copy(gate_hbm.at[0], gate_w, weight_sems.at[0]),
        pltpu.make_async_copy(linear_hbm.at[0], linear_w, weight_sems.at[1]),
        pltpu.make_async_copy(down_hbm.at[0], down_w, weight_sems.at[2]),
    ]
    for fetch in fetches:
        fetch.start()

    share, model = middle_ref.shape
    length = meta_ref.shape[0]
    slots = rows_out.shape[1]
    pick = (iota((length, share), 0) == tp * share + iota((length, share), 1)).astype(f32)
    facts = exact_dot(meta_ref[...], pick, ((0,), (0,)))
    expert = iota((n_sp, share), 0).astype(f32)
    first, second = facts[0:1] == expert, facts[1:2] == expert
    uses = jnp.where(first, 1.0, 0.0) + jnp.where(second, 1.0, 0.0)
    weights = jnp.where(first, facts[2:3], 0.0) + jnp.where(second, facts[3:4], 0.0)
    before = (iota((share, share), 0) < iota((share, share), 1)).astype(bf16)
    rank = jnp.dot(uses.astype(bf16), before, preferred_element_type=f32)
    slot = iota((slots, share), 0).astype(f32)
    chosen = [
        jnp.where(slot == rank[e : e + 1], uses[e : e + 1], 0.0) for e in range(n_sp)
    ]
    weigh = jnp.concatenate([chosen[e] * weights[e : e + 1] for e in range(n_sp)], axis=0)
    chosen = jnp.concatenate(chosen, axis=0).astype(bf16)
    rows = jnp.dot(chosen, middle_ref[...].astype(bf16), preferred_element_type=f32)
    for e in range(n_sp):
        rows_out[e] = rows[e * slots : (e + 1) * slots].astype(bf16)

    pl.semaphore_wait(barrier, n_sp - 1 + n_tp - 1)

    def remote(src, dst, send, receive, where):
        return pltpu.make_async_remote_copy(
            src_ref=src, dst_ref=dst, send_sem=send, recv_sem=receive, device_id=where
        )

    def plus(k):
        return lax.rem(sp + k, n_sp)

    def minus(k):
        return lax.rem(sp + n_sp - k, n_sp)

    def up(k):
        return lax.rem(hi + k, n_hi)

    sends = []

    def go(copy):
        copy.start()
        sends.append(copy)

    for k in range(1, n_sp):
        e = plus(k)
        go(remote(rows_out.at[e], recv.at[tp, sp], s1.at[k], r1.at[sp], {"sp": e}))
    recv[tp, sp] = rows_out[sp]

    def landed(m, s, sem):
        remote(rows_out.at[0], recv.at[m, s], s1.at[0], sem, {"sp": plus(1)}).wait_recv()

    def to_sibling(h, s):
        block = recv.at[h * 2 + lo, s]
        go(remote(block, block, s2d.at[h, s], r2.at[h * 2 + lo, s], {"tp": sibling}))

    def pass_own(s):
        for k in range(1, n_hi):
            h = up(k)
            block = recv.at[tp, s]
            go(remote(block, block, s2x.at[h, s], r2.at[tp, s], {"tp": h * 2 + lo}))
        to_sibling(hi, s)

    pass_own(sp)
    for k in range(1, n_sp):
        s = minus(k)
        landed(tp, s, r1.at[s])
        pass_own(s)
    for k in range(1, n_hi):
        h = up(k)
        for j in range(n_sp):
            s = minus(j)
            landed(h * 2 + lo, s, r2.at[h * 2 + lo, s])
            to_sibling(h, s)
    for fetch in fetches:
        fetch.wait()

    def flat(block):
        return block.astype(f32).reshape(n_sp * slots, model).astype(bf16)

    def compute(g):
        x = flat(recv[g])
        a = jnp.dot(x, gate_w[...], preferred_element_type=f32)
        b = jnp.dot(x, linear_w[...], preferred_element_type=f32)
        hidden = (jax.nn.silu(a) * b).astype(bf16)
        y = jnp.dot(hidden, down_w[...], preferred_element_type=f32)
        part[g] = y.reshape(n_sp, slots, model).astype(bf16)

    def give(h):
        go(remote(part.at[h * 2 + 1 - lo], sib.at[h], s3.at[h], r3.at[h], {"tp": sibling}))

    def given(h):
        remote(part.at[0], sib.at[h], s3.at[h], r3.at[h], {"tp": sibling}).wait_recv()

    compute(tp)
    for j in range(n_sp):
        s = minus(j)
        landed(sibling, s, r2.at[sibling, s])
    compute(sibling)
    give(hi)
    for k in range(1, n_hi):
        h = up(k)
        other = h * 2 + 1 - lo
        for j in range(n_sp):
            s = minus(j)
            landed(other, s, r2.at[other, s])
        compute(other)
        give(h)
        compute(h * 2 + lo)
        given(h)
        for j in range(n_sp):
            s = plus(j)
            pair[h, s] = (part[h * 2 + lo, s].astype(f32) + sib[h, s].astype(f32)).astype(bf16)
            go(
                remote(
                    pair.at[h, s],
                    peer_sum.at[hi, s],
                    s4.at[h, s],
                    r4.at[hi, s],
                    {"tp": h * 2 + lo},
                )
            )
    given(hi)
    for j in range(n_sp):
        s = plus(j)
        value = part[tp, s].astype(f32) + sib[hi, s].astype(f32)
        for k in range(1, n_hi):
            h = up(k)
            remote(
                pair.at[0, 0], peer_sum.at[h, s], s4.at[0, 0], r4.at[h, s], {"tp": sibling}
            ).wait_recv()
            value = value + peer_sum[h, s].astype(f32)
        if j == 0:
            back[sp] = value.astype(bf16)
        else:
            final[s] = value.astype(bf16)
            go(remote(final.at[s], back.at[sp], s5.at[j], r5.at[sp], {"sp": s}))
    coarse = weigh.astype(bf16)
    fine = (weigh - coarse.astype(f32)).astype(bf16)
    for j in range(1, n_sp):
        s = minus(j)
        remote(final.at[0], back.at[s], s5.at[0], r5.at[s], {"sp": plus(1)}).wait_recv()
    answers = flat(back[...])
    over = (((0,), (0,)), ((), ()))
    routed = lax.dot_general(coarse, answers, over, preferred_element_type=f32)
    routed = routed + lax.dot_general(fine, answers, over, preferred_element_type=f32)
    out_ref[...] = layer_norm(deep_alpha * middle_ref[...] + routed, gain_ref[...]).astype(bf16)
    for copy in sends:
        copy.wait_send()


def experts_layer(middle, meta, gain, gate_weight, linear_weight, down_weight, n_sp, n_tp, slots):
    share, model = middle.shape
    hidden = gate_weight.shape[2]
    n_hi = n_tp // 2
    vmem = pl.BlockSpec(memory_space=pltpu.VMEM)
    hbm = pl.BlockSpec(memory_space=pl.ANY)
    dma = pltpu.SemaphoreType.DMA
    block = (n_sp, slots, model)
    return pl.pallas_call(
        functools.partial(experts_kernel, n_sp, n_tp),
        out_shape=jax.ShapeDtypeStruct((share, model), bf16),
        in_specs=[vmem] * 3 + [hbm] * 3,
        out_specs=vmem,
        scratch_shapes=[
            pltpu.VMEM(block, bf16),
            pltpu.VMEM((n_tp,) + block, bf16),
            pltpu.VMEM((n_tp,) + block, bf16),
            pltpu.VMEM((n_hi,) + block, bf16),
            pltpu.VMEM((n_hi,) + block, bf16),
            pltpu.VMEM((n_hi,) + block, bf16),
            pltpu.VMEM(block, bf16),
            pltpu.VMEM(block, bf16),
            pltpu.VMEM((model, hidden), bf16),
            pltpu.VMEM((model, hidden), bf16),
            pltpu.VMEM((hidden, model), bf16),
            dma((3,)),
            dma((n_sp,)),
            dma((n_sp,)),
            dma((n_hi, n_sp)),
            dma((n_hi, n_sp)),
            dma((n_tp, n_sp)),
            dma((n_hi,)),
            dma((n_hi,)),
            dma((n_hi, n_sp)),
            dma((n_hi, n_sp)),
            dma((n_sp,)),
            dma((n_sp,)),
        ],
        compiler_params=pltpu.CompilerParams(
            collective_id=1, has_side_effects=True, vmem_limit_bytes=60 * 2**20
        ),
        name="experts",
    )(middle, meta, gain[None, :], gate_weight, linear_weight, down_weight)


def on_device(
    residual,
    mixer_input,
    log_gate,
    decay_rate,
    turn_rate,
    drive_real,
    drive_imaginary,
    read_real,
    read_imaginary,
    skip_gain,
    project_weight,
    norm_gain,
    final_gain,
    routes,
    group_weight,
    expert_weight,
    gate_weight,
    linear_weight,
    down_weight,
):
    experts = lax.axis_size("sp")
    members = lax.axis_size("tp")
    middle = mixer(
        (
            residual,
            mixer_input,
            log_gate,
            decay_rate,
            turn_rate,
            drive_real,
            drive_imaginary,
            read_real,
            read_imaginary,
            skip_gain,
            project_weight,
            norm_gain,
        ),
        experts,
        members,
    )
    share = residual.shape[0]
    top = routes.shape[1]
    slots = max(2, 3 * share * top // (2 * experts))
    slots = -(-slots // 8) * 8
    mixing = group_weight[:, None] * expert_weight / jnp.sum(expert_weight, axis=1, keepdims=True)
    meta = jnp.concatenate([routes.astype(f32), mixing], axis=1)
    return experts_layer(
        middle,
        meta,
        final_gain,
        gate_weight,
        linear_weight,
        down_weight,
        experts,
        members,
        slots,
    )


def solution(mesh):
    placed = (
        P(("sp", "tp"), None),
        P("sp", "tp"),
        P("sp", "tp"),
        P(None, "tp", None),
        P(None, "tp", None),
        P(None, "tp", None, None),
        P(None, "tp", None, None),
        P(None, "tp", None, None),
        P(None, "tp", None, None),
        P("tp"),
        P(),
        P(),
        P(),
        P("sp", None),
        P("sp"),
        P("sp", None),
        P("sp", None, "tp"),
        P("sp", None, "tp"),
        P("sp", "tp", None),
    )
    return jax.shard_map(
        on_device, mesh=mesh, in_specs=placed, out_specs=P(("sp", "tp"), None), check_vma=False
    )
```

```python
import functools

import jax
import jax.numpy as jnp
from jax import lax
from jax.experimental import pallas as pl
from jax.experimental.pallas import tpu as pltpu
from jax.sharding import PartitionSpec as P

deep_alpha = 2.0**0.25
norm_epsilon = 1e-05
highest = lax.Precision.HIGHEST
f32 = jnp.float32
bf16 = jnp.bfloat16
segments = 8


def layer_norm(values, gain):
    center = values - jnp.mean(values, axis=-1, keepdims=True)
    spread = jnp.mean(center * center, axis=-1, keepdims=True)
    return center * lax.rsqrt(spread + norm_epsilon) * gain


def iota(shape, axis):
    return lax.broadcasted_iota(jnp.int32, shape, axis)


def exact_dot(a, b, dims=((1,), (0,))):
    return lax.dot_general(a, b, (dims, ((), ())), precision=highest, preferred_element_type=f32)


def mixer_kernel(n_sp, n_tp, *refs):
    sources, middle_ref, staged = refs[:12], refs[12], refs[13:25]
    (push, gate, seg, enter, total, totals, act, chan) = refs[25:33]
    (stage_sems, send_a, recv_a, send_b, recv_b) = refs[33:]
    loads = [
        pltpu.make_async_copy(source, place, stage_sems.at[i])
        for i, (source, place) in enumerate(zip(sources, staged))
    ]
    for load in loads:
        load.start()
    (x_ref, gate_ref, decay_ref, turn_ref, drive_re, drive_im) = staged[:6]
    (read_re, read_im, skip_ref, residual_ref, gain_ref, weight) = staged[6:]
    sp = lax.axis_index("sp")
    tp = lax.axis_index("tp")
    barrier = pltpu.get_barrier_semaphore()
    for k in range(1, n_sp):
        pl.semaphore_signal(barrier, inc=1, device_id={"sp": lax.rem(sp + k, n_sp)})
    for k in range(1, n_tp):
        pl.semaphore_signal(barrier, inc=1, device_id={"tp": lax.rem(tp + k, n_tp)})
    for load in loads[:6]:
        load.wait()

    length, channels = x_ref.shape
    groups, states = decay_ref.shape[1:]
    width = groups * states
    each = channels // groups
    steps = length // segments
    order = iota((length, length), 0)
    place = iota((length, length), 1)
    shuffle = (place == (order % segments) * steps + order // segments).astype(f32)
    x = jnp.dot(shuffle.astype(bf16), x_ref[...], preferred_element_type=f32)
    spread = (iota((states, width), 1) % states == iota((states, width), 0)).astype(f32)
    own = iota((groups, width), 1) // states == iota((groups, width), 0)
    diagonal = iota((channels, width), 1) // states == iota((channels, width), 0) // each

    def row(values):
        wide = exact_dot(values, spread)
        return jnp.sum(jnp.where(own, wide, 0.0), axis=0, keepdims=True)

    def table(values):
        return jnp.where(diagonal, exact_dot(values, spread), 0.0)

    gate[...] = exact_dot(exact_dot(shuffle, jnp.exp(gate_ref[...])), own.astype(f32))
    turn_rows = []
    for k in range(2):
        rate = decay_ref[k]
        turn = turn_ref[k]
        retain = jnp.exp(-rate)
        scale = row(jnp.sqrt(1.0 - jnp.exp(-2.0 * rate)))
        turn_rows.append((row(retain * jnp.cos(turn)), row(retain * jnp.sin(turn))))
        push[2 * k] = exact_dot(x, table(drive_re[k]) * scale)
        push[2 * k + 1] = exact_dot(x, table(drive_im[k]) * scale)
    (f_re, f_im), (b_re, b_im) = turn_rows

    zero = jnp.zeros((segments, width), f32)
    one = jnp.ones((segments, width), f32)

    def rows_of(j):
        return pl.ds(pl.multiple_of(j * segments, segments), segments)

    def first(j, c):
        out = []
        for k, (sr, si) in enumerate(((f_re, f_im), (b_re, b_im))):
            at = rows_of(j if k == 0 else steps - 1 - j)
            ar, ai, vr, vi = c[4 * k : 4 * k + 4]
            g = gate[at, :]
            mr, mi = g * sr, g * si
            out += [
                mr * ar - mi * ai,
                mr * ai + mi * ar,
                mr * vr - mi * vi + push[2 * k, at, :],
                mr * vi + mi * vr + push[2 * k + 1, at, :],
            ]
        return tuple(out)

    ends = lax.fori_loop(0, steps, first, (one, zero, zero, zero) * 2)
    for i, part in enumerate(ends):
        seg[i] = part

    def link(parts, c):
        ar, ai, vr, vi = parts
        return (ar * c[0] - ai * c[1] + vr, ar * c[1] + ai * c[0] + vi)

    def seg_rows(k, s):
        return [seg[4 * k + i, s : s + 1, :] for i in range(4)]

    for k in range(2):
        span = range(segments) if k == 0 else range(segments - 1, -1, -1)
        decay = (one[:1], zero[:1])
        state = (zero[:1], zero[:1])
        for s in span:
            parts = seg_rows(k, s)
            state = link(parts, state)
            decay = link(parts[:2] + [0.0, 0.0], decay)
        for i, value in enumerate(decay + state):
            total[4 * k + i : 4 * k + i + 1, :] = value
    totals[sp] = total[...]

    pl.semaphore_wait(barrier, n_sp - 1 + n_tp - 1)

    def hand(k):
        peer = lax.rem(sp + k, n_sp)
        return pltpu.make_async_remote_copy(
            src_ref=total,
            dst_ref=totals.at[sp],
            send_sem=send_a.at[k],
            recv_sem=recv_a.at[sp],
            device_id={"sp": peer},
        )

    def arrival(k):
        source = lax.rem(sp + k, n_sp)
        return pltpu.make_async_remote_copy(
            src_ref=total,
            dst_ref=totals.at[source],
            send_sem=send_a.at[k],
            recv_sem=recv_a.at[source],
            device_id={"sp": source},
        )

    for k in range(1, n_sp):
        hand(k).start()
    for load in loads[6:9]:
        load.wait()
    tables = [(table(read_re[k]), table(read_im[k])) for k in range(2)]
    for k in range(1, n_sp):
        arrival(k).wait_recv()

    for k in range(2):
        c = (zero[:1], zero[:1])
        for d in range(n_sp) if k == 0 else range(n_sp - 1, -1, -1):
            new = link([totals[d, 4 * k + i : 4 * k + i + 1, :] for i in range(4)], c)
            counts = d < sp if k == 0 else d > sp
            c = tuple(jnp.where(counts, a, b) for a, b in zip(new, c))
        for s in range(segments) if k == 0 else range(segments - 1, -1, -1):
            enter[2 * k, s : s + 1, :] = c[0]
            enter[2 * k + 1, s : s + 1, :] = c[1]
            c = link(seg_rows(k, s), c)

    def second(j, c):
        out = []
        for k, (sr, si) in enumerate(((f_re, f_im), (b_re, b_im))):
            at = rows_of(j if k == 0 else steps - 1 - j)
            vr, vi = c[2 * k : 2 * k + 2]
            g = gate[at, :]
            mr, mi = g * sr, g * si
            new_re = mr * vr - mi * vi + push[2 * k, at, :]
            new_im = mr * vi + mi * vr + push[2 * k + 1, at, :]
            push[2 * k, at, :] = new_re
            push[2 * k + 1, at, :] = new_im
            out += [new_re, new_im]
        return tuple(out)

    lax.fori_loop(0, steps, second, tuple(enter[i] for i in range(4)))
    over = ((1,), (1,))
    readout = exact_dot(push[0], tables[0][0], over) - exact_dot(push[1], tables[0][1], over)
    readout = readout + (
        exact_dot(push[2], tables[1][0], over) - exact_dot(push[3], tables[1][1], over)
    )
    readout = readout + skip_ref[...] * x
    mixed = jax.nn.gelu(readout).astype(bf16)
    act[...] = lax.dot_general(
        shuffle.astype(bf16), mixed, (((0,), (0,)), ((), ())), preferred_element_type=f32
    ).astype(bf16)

    share = length // n_tp

    def shift(k, out):
        peer = lax.rem(tp + k, n_tp)
        return pltpu.make_async_remote_copy(
            src_ref=act.at[pl.ds(pl.multiple_of(peer * share, share), share)],
            dst_ref=chan.at[tp if out else peer],
            send_sem=send_b.at[k],
            recv_sem=recv_b.at[tp if out else peer],
            device_id={"tp": peer},
        )

    for k in range(1, n_tp):
        shift(k, True).start()
    chan[tp] = act[pl.ds(pl.multiple_of(tp * share, share), share), :]
    for load in loads[9:]:
        load.wait()
    for k in range(1, n_tp):
        shift(k, False).wait_recv()
    whole = jnp.concatenate([chan[m] for m in range(n_tp)], axis=1)
    branch = jnp.dot(whole, weight[...], preferred_element_type=f32)
    middle_ref[...] = layer_norm(
        deep_alpha * residual_ref[...].astype(f32) + branch, gain_ref[...]
    )
    for k in range(1, n_sp):
        hand(k).wait_send()
    for k in range(1, n_tp):
        shift(k, True).wait_send()


def mixer(args, n_sp, n_tp):
    (residual, x, log_gate, decay, turn, d_re, d_im, r_re, r_im, skip, weight, gain) = args
    length, channels = x.shape
    groups, states = decay.shape[1:]
    width = groups * states
    share, model = residual.shape
    flat = lambda a: a.reshape(2, channels, states)
    operands = (x, log_gate, decay, turn, flat(d_re), flat(d_im), flat(r_re), flat(r_im))
    operands += (skip[None, :], residual, gain[None, :], weight)
    vmem = pl.BlockSpec(memory_space=pltpu.VMEM)
    dma = pltpu.SemaphoreType.DMA
    return pl.pallas_call(
        functools.partial(mixer_kernel, n_sp, n_tp),
        out_shape=jax.ShapeDtypeStruct((share, model), f32),
        in_specs=[pl.BlockSpec(memory_space=pl.ANY)] * len(operands),
        out_specs=vmem,
        scratch_shapes=[pltpu.VMEM(a.shape, a.dtype) for a in operands]
        + [
            pltpu.VMEM((4, length, width), f32),
            pltpu.VMEM((length, width), f32),
            pltpu.VMEM((8, segments, width), f32),
            pltpu.VMEM((4, segments, width), f32),
            pltpu.VMEM((8, width), f32),
            pltpu.VMEM((n_sp, 8, width), f32),
            pltpu.VMEM((length, channels), bf16),
            pltpu.VMEM((n_tp, share, channels), bf16),
            dma((len(operands),)),
            dma((n_sp,)),
            dma((n_sp,)),
            dma((n_tp,)),
            dma((n_tp,)),
        ],
        compiler_params=pltpu.CompilerParams(
            collective_id=0, has_side_effects=True, vmem_limit_bytes=60 * 2**20
        ),
        name="mixer",
    )(*operands)


def experts_kernel(
    n_sp,
    n_tp,
    middle_ref,
    meta_ref,
    gain_ref,
    gate_hbm,
    linear_hbm,
    down_hbm,
    out_ref,
    rows_out,
    recv,
    part,
    sib,
    pair,
    peer_sum,
    final,
    back,
    gate_w,
    linear_w,
    down_w,
    weight_sems,
    s1,
    r1,
    s2x,
    s2d,
    r2,
    s3,
    r3,
    s4,
    r4,
    s5,
    r5,
):
    sp = lax.axis_index("sp")
    tp = lax.axis_index("tp")
    n_hi = n_tp // 2
    hi = tp // 2
    lo = tp % 2
    sibling = hi * 2 + 1 - lo
    barrier = pltpu.get_barrier_semaphore()
    for k in range(1, n_sp):
        pl.semaphore_signal(barrier, inc=1, device_id={"sp": lax.rem(sp + k, n_sp)})
    for k in range(1, n_tp):
        pl.semaphore_signal(barrier, inc=1, device_id={"tp": lax.rem(tp + k, n_tp)})
    fetches = [
        pltpu.make_async_copy(gate_hbm.at[0], gate_w, weight_sems.at[0]),
        pltpu.make_async_copy(linear_hbm.at[0], linear_w, weight_sems.at[1]),
        pltpu.make_async_copy(down_hbm.at[0], down_w, weight_sems.at[2]),
    ]
    for fetch in fetches:
        fetch.start()

    share, model = middle_ref.shape
    length = meta_ref.shape[0]
    slots = rows_out.shape[1]
    room = -(-slots // 8) * 8
    pick = (iota((length, share), 0) == tp * share + iota((length, share), 1)).astype(f32)
    facts = exact_dot(meta_ref[...], pick, ((0,), (0,)))
    expert = iota((n_sp, share), 0).astype(f32)
    first, second = facts[0:1] == expert, facts[1:2] == expert
    uses = jnp.where(first, 1.0, 0.0) + jnp.where(second, 1.0, 0.0)
    weights = jnp.where(first, facts[2:3], 0.0) + jnp.where(second, facts[3:4], 0.0)
    before = (iota((share, share), 0) < iota((share, share), 1)).astype(bf16)
    rank = jnp.dot(uses.astype(bf16), before, preferred_element_type=f32)
    slot = iota((room, share), 0).astype(f32)
    chosen = [
        jnp.where(slot == rank[e : e + 1], uses[e : e + 1], 0.0) for e in range(n_sp)
    ]
    weigh = jnp.concatenate([chosen[e] * weights[e : e + 1] for e in range(n_sp)], axis=0)
    chosen = jnp.concatenate(chosen, axis=0).astype(bf16)
    rows = jnp.dot(chosen, middle_ref[...].astype(bf16), preferred_element_type=f32)
    for e in range(n_sp):
        rows_out[e] = rows[e * room : e * room + slots].astype(bf16)

    pl.semaphore_wait(barrier, n_sp - 1 + n_tp - 1)

    def remote(src, dst, send, receive, where):
        return pltpu.make_async_remote_copy(
            src_ref=src, dst_ref=dst, send_sem=send, recv_sem=receive, device_id=where
        )

    def plus(k):
        return lax.rem(sp + k, n_sp)

    def minus(k):
        return lax.rem(sp + n_sp - k, n_sp)

    def up(k):
        return lax.rem(hi + k, n_hi)

    sends = []

    def go(copy):
        copy.start()
        sends.append(copy)

    for k in range(1, n_sp):
        e = plus(k)
        go(remote(rows_out.at[e], recv.at[tp, sp], s1.at[k], r1.at[sp], {"sp": e}))
    recv[tp, sp] = rows_out[sp]

    def landed(m, s, sem):
        remote(rows_out.at[0], recv.at[m, s], s1.at[0], sem, {"sp": plus(1)}).wait_recv()

    def to_sibling(h, s):
        block = recv.at[h * 2 + lo, s]
        go(remote(block, block, s2d.at[h, s], r2.at[h * 2 + lo, s], {"tp": sibling}))

    def pass_own(s):
        for k in range(1, n_hi):
            h = up(k)
            block = recv.at[tp, s]
            go(remote(block, block, s2x.at[h, s], r2.at[tp, s], {"tp": h * 2 + lo}))
        to_sibling(hi, s)

    pass_own(sp)
    for k in range(1, n_sp):
        s = minus(k)
        landed(tp, s, r1.at[s])
        pass_own(s)
    for k in range(1, n_hi):
        h = up(k)
        for j in range(n_sp):
            s = minus(j)
            landed(h * 2 + lo, s, r2.at[h * 2 + lo, s])
            to_sibling(h, s)
    for fetch in fetches:
        fetch.wait()

    def flat(block):
        block = block.astype(f32)
        if room > slots:
            blank = jnp.zeros((n_sp, room - slots, model), f32)
            block = jnp.concatenate([block, blank], axis=1)
        return block.reshape(n_sp * room, model).astype(bf16)

    def compute(g):
        x = flat(recv[g])
        a = jnp.dot(x, gate_w[...], preferred_element_type=f32)
        b = jnp.dot(x, linear_w[...], preferred_element_type=f32)
        hidden = (jax.nn.silu(a) * b).astype(bf16)
        y = jnp.dot(hidden, down_w[...], preferred_element_type=f32)
        part[g] = y.reshape(n_sp, room, model)[:, :slots].astype(bf16)

    def give(h):
        go(remote(part.at[h * 2 + 1 - lo], sib.at[h], s3.at[h], r3.at[h], {"tp": sibling}))

    def given(h):
        remote(part.at[0], sib.at[h], s3.at[h], r3.at[h], {"tp": sibling}).wait_recv()

    compute(tp)
    for j in range(n_sp):
        s = minus(j)
        landed(sibling, s, r2.at[sibling, s])
    compute(sibling)
    give(hi)
    for k in range(1, n_hi):
        h = up(k)
        other = h * 2 + 1 - lo
        for j in range(n_sp):
            s = minus(j)
            landed(other, s, r2.at[other, s])
        compute(other)
        give(h)
        compute(h * 2 + lo)
        given(h)
        for j in range(n_sp):
            s = plus(j)
            pair[h, s] = (part[h * 2 + lo, s].astype(f32) + sib[h, s].astype(f32)).astype(bf16)
            go(
                remote(
                    pair.at[h, s],
                    peer_sum.at[hi, s],
                    s4.at[h, s],
                    r4.at[hi, s],
                    {"tp": h * 2 + lo},
                )
            )
    given(hi)
    for j in range(n_sp):
        s = plus(j)
        value = part[tp, s].astype(f32) + sib[hi, s].astype(f32)
        for k in range(1, n_hi):
            h = up(k)
            remote(
                pair.at[0, 0], peer_sum.at[h, s], s4.at[0, 0], r4.at[h, s], {"tp": sibling}
            ).wait_recv()
            value = value + peer_sum[h, s].astype(f32)
        if j == 0:
            back[sp] = value.astype(bf16)
        else:
            final[s] = value.astype(bf16)
            go(remote(final.at[s], back.at[sp], s5.at[j], r5.at[sp], {"sp": s}))
    coarse = weigh.astype(bf16)
    fine = (weigh - coarse.astype(f32)).astype(bf16)
    for j in range(1, n_sp):
        s = minus(j)
        remote(final.at[0], back.at[s], s5.at[0], r5.at[s], {"sp": plus(1)}).wait_recv()
    answers = flat(back[...])
    over = (((0,), (0,)), ((), ()))
    routed = lax.dot_general(coarse, answers, over, preferred_element_type=f32)
    routed = routed + lax.dot_general(fine, answers, over, preferred_element_type=f32)
    out_ref[...] = layer_norm(deep_alpha * middle_ref[...] + routed, gain_ref[...]).astype(bf16)
    for copy in sends:
        copy.wait_send()


def experts_layer(middle, meta, gain, gate_weight, linear_weight, down_weight, n_sp, n_tp, slots):
    share, model = middle.shape
    hidden = gate_weight.shape[2]
    n_hi = n_tp // 2
    vmem = pl.BlockSpec(memory_space=pltpu.VMEM)
    hbm = pl.BlockSpec(memory_space=pl.ANY)
    dma = pltpu.SemaphoreType.DMA
    block = (n_sp, slots, model)
    return pl.pallas_call(
        functools.partial(experts_kernel, n_sp, n_tp),
        out_shape=jax.ShapeDtypeStruct((share, model), bf16),
        in_specs=[vmem] * 3 + [hbm] * 3,
        out_specs=vmem,
        scratch_shapes=[
            pltpu.VMEM(block, bf16),
            pltpu.VMEM((n_tp,) + block, bf16),
            pltpu.VMEM((n_tp,) + block, bf16),
            pltpu.VMEM((n_hi,) + block, bf16),
            pltpu.VMEM((n_hi,) + block, bf16),
            pltpu.VMEM((n_hi,) + block, bf16),
            pltpu.VMEM(block, bf16),
            pltpu.VMEM(block, bf16),
            pltpu.VMEM((model, hidden), bf16),
            pltpu.VMEM((model, hidden), bf16),
            pltpu.VMEM((hidden, model), bf16),
            dma((3,)),
            dma((n_sp,)),
            dma((n_sp,)),
            dma((n_hi, n_sp)),
            dma((n_hi, n_sp)),
            dma((n_tp, n_sp)),
            dma((n_hi,)),
            dma((n_hi,)),
            dma((n_hi, n_sp)),
            dma((n_hi, n_sp)),
            dma((n_sp,)),
            dma((n_sp,)),
        ],
        compiler_params=pltpu.CompilerParams(
            collective_id=1, has_side_effects=True, vmem_limit_bytes=60 * 2**20
        ),
        name="experts",
    )(middle, meta, gain[None, :], gate_weight, linear_weight, down_weight)


def on_device(
    residual,
    mixer_input,
    log_gate,
    decay_rate,
    turn_rate,
    drive_real,
    drive_imaginary,
    read_real,
    read_imaginary,
    skip_gain,
    project_weight,
    norm_gain,
    final_gain,
    routes,
    group_weight,
    expert_weight,
    gate_weight,
    linear_weight,
    down_weight,
):
    experts = lax.axis_size("sp")
    members = lax.axis_size("tp")
    middle = mixer(
        (
            residual,
            mixer_input,
            log_gate,
            decay_rate,
            turn_rate,
            drive_real,
            drive_imaginary,
            read_real,
            read_imaginary,
            skip_gain,
            project_weight,
            norm_gain,
        ),
        experts,
        members,
    )
    share = residual.shape[0]
    top = routes.shape[1]
    slots = max(2, 3 * share * top // (2 * experts))
    mixing = group_weight[:, None] * expert_weight / jnp.sum(expert_weight, axis=1, keepdims=True)
    meta = jnp.concatenate([routes.astype(f32), mixing], axis=1)
    return experts_layer(
        middle,
        meta,
        final_gain,
        gate_weight,
        linear_weight,
        down_weight,
        experts,
        members,
        slots,
    )


def solution(mesh):
    placed = (
        P(("sp", "tp"), None),
        P("sp", "tp"),
        P("sp", "tp"),
        P(None, "tp", None),
        P(None, "tp", None),
        P(None, "tp", None, None),
        P(None, "tp", None, None),
        P(None, "tp", None, None),
        P(None, "tp", None, None),
        P("tp"),
        P(),
        P(),
        P(),
        P("sp", None),
        P("sp"),
        P("sp", None),
        P("sp", None, "tp"),
        P("sp", None, "tp"),
        P("sp", "tp", None),
    )
    return jax.shard_map(
        on_device, mesh=mesh, in_specs=placed, out_specs=P(("sp", "tp"), None), check_vma=False
    )
```
